32 devices in a mesh: fs: 8 (over z, y), tp: 4 (over x, core).
Axes of the slice: x: 2, y: 2, z: 4, core: 2. Of those that a mesh axis runs over, the one named last changes fastest.
Arguments:
- later_input: bfloat16 [4096, 2048], P(('fs', 'tp')), may hold values from -6 to 6
- earlier_input: bfloat16 [4096, 2048], P('fs'), may hold values from -6 to 6
- earlier_hidden: bfloat16 [4096, 4096], P('fs', 'tp'), may hold values from -6 to 6
- cotangent: bfloat16 [4096, 2048], P('fs'), may hold values from -6 to 6
- up_weight: bfloat16 [2048, 4096], P('fs', 'tp'), may hold values from -0.125 to 0.125
- down_weight: bfloat16 [4096, 2048], P(('tp', 'fs')), may hold values from -0.09375 to 0.09375
- up_sum: float32 [2048, 4096], P('fs', 'tp'), may hold values from -4 to 4
- down_sum: float32 [4096, 2048], P(('tp', 'fs')), may hold values from -4 to 4
Outputs:
- later_output: bfloat16 [4096, 2048], P(('fs', 'tp'))
- later_hidden: bfloat16 [4096, 4096], P('fs', 'tp')
- earlier_grad: bfloat16 [4096, 2048], P(('fs', 'tp'))
- up_sum_next: float32 [2048, 4096], P('fs', 'tp')
- down_sum_next: float32 [4096, 2048], P(('tp', 'fs'))
The draws below stay inside these ranges and needn't reach their ends.
All inputs are finite; a program needn't handle non-finite values.
Results may differ from the reference program's by a relative error of at most 0.0095.
Values may be sent and summed in bfloat16 or wider, within the bound.
No kernel may reach another device: no remote copies, remote signals or barrier semaphores. Data moves between devices by JAX's collectives and lax.ppermute only.
A program may use at most 128 MiB of HBM per device.

```python
import jax
import jax.numpy as jnp
from jax import lax

D = 2048
FF = 4096
TOKENS = 4096
N_FS = 8
N_TP = 4


def spiked(entries, key, source, target, shards_of, factor):
    owner, partner = [(jnp.arange(entries.shape[dim]) // (entries.shape[dim] // shards_of)).reshape([-1 if axis == dim else 1 for axis in range(entries.ndim)]) for dim in (source, target)]
    chosen = jax.random.permutation(key, shards_of)[partner]
    strong = (owner == chosen) | (owner == (partner + shards_of // 2) % shards_of)
    return jnp.where(strong, factor * entries, entries)


def shard_levels(key, shape, split, low, largest):
    loudness = 1.0
    for dim, blocks in split:
        heights = jax.random.uniform(jax.random.fold_in(jax.random.fold_in(key, 6), dim), (blocks,), jnp.float32, low / len(split), largest / len(split))
        loudness = loudness * jnp.repeat(jnp.exp(heights), shape[dim] // blocks).reshape((-1,) + (1,) * (len(shape) - 1 - dim))
    return loudness


def scatter_about(key, shape, deviation, reach, split=(), held_as=jnp.bfloat16):
    entries = jax.random.normal(key, shape, jnp.float32) * deviation
    if len(split) > 0:
        entries = shard_levels(key, shape, split, -0.22, 0.18) * entries
    return jnp.clip(entries, min=-reach, max=reach).astype(held_as)


def heavy_noise(own_key, shape, scale, reach, cuts, heavy, kind=jnp.bfloat16):
    array = scale * jax.random.normal(own_key, shape, jnp.float32)
    if cuts:
        array = array * shard_levels(own_key, shape, cuts, -0.22, 0.18)
    return jnp.clip(spiked(array, jax.random.fold_in(own_key, 3), *heavy), -reach, reach).astype(kind)


def setup_inputs(seed: int = 0) -> dict:
    arg_keys = jax.random.split(jax.random.key(seed), 9)
    later_input = scatter_about(arg_keys[0], (TOKENS, D), 1.0, 6.0, ((0, 32),))
    earlier_input = heavy_noise(arg_keys[1], (TOKENS, D), 1.0, 6.0, ((0, 8),), (0, 1, 8, 2.0))
    earlier_hidden = scatter_about(arg_keys[2], (TOKENS, FF), 1.0, 6.0, ((0, 8), (1, 4)))
    cotangent = heavy_noise(arg_keys[3], (TOKENS, D), 1.0, 6.0, ((0, 8),), (0, 1, 8, 2.0))
    up_weight = scatter_about(arg_keys[4], (D, FF), D ** -0.5, 0.125, ((0, 8), (1, 4)))
    down_weight = scatter_about(arg_keys[5], (FF, D), FF ** -0.5, 0.09375, ((0, 32),))
    up_sum = scatter_about(arg_keys[6], (D, FF), 0.5, 4.0, ((0, 8), (1, 4)), jnp.float32)
    down_sum = scatter_about(arg_keys[7], (FF, D), 0.5, 4.0, ((0, 32),), jnp.float32)
    return dict(later_input=later_input, earlier_input=earlier_input, earlier_hidden=earlier_hidden, cotangent=cotangent, up_weight=up_weight, down_weight=down_weight, up_sum=up_sum, down_sum=down_sum)


def squared_relu(pre_values):
    lifted = jnp.maximum(pre_values.astype(jnp.float32), 0.0)
    return lifted, lifted * lifted


def rounded_split_sum(left_rows, right_rows):
    span_width = left_rows.shape[1] // N_TP
    running = jnp.zeros((left_rows.shape[0], right_rows.shape[1]), jnp.float32)
    for block_index in range(N_TP):
        lower_edge = block_index * span_width
        upper_edge = lower_edge + span_width
        partial_value = jnp.dot(left_rows[:, lower_edge:upper_edge], right_rows[lower_edge:upper_edge],
                          preferred_element_type=jnp.float32)
        rounded = lax.optimization_barrier(partial_value.astype(jnp.bfloat16))
        running = running + rounded.astype(jnp.float32)
    return running.astype(jnp.bfloat16)


def reference(later_input, earlier_input, earlier_hidden, cotangent, up_weight, down_weight, up_sum, down_sum):
    later_hidden = jnp.dot(later_input, up_weight, preferred_element_type=jnp.float32).astype(jnp.bfloat16)
    lifted_later, squared_later = squared_relu(later_hidden)
    later_output = rounded_split_sum(squared_later.astype(jnp.bfloat16), down_weight)
    row_total = earlier_input.shape[0]
    grad_scale = float(row_total) ** -0.5
    group_rows = row_total // N_FS

    def backward_block(totals, pieces):
        inputs, hidden, upstream = pieces
        lifted, squared = squared_relu(hidden)
        activation = squared.astype(jnp.bfloat16)
        act_slope = jnp.dot(upstream, down_weight.T, preferred_element_type=jnp.float32)
        pre_grad = (2.0 * act_slope * lifted).astype(jnp.bfloat16)
        up_total = totals[0] + jnp.dot(inputs.T, pre_grad, preferred_element_type=jnp.float32)
        down_total = totals[1] + jnp.dot(activation.T, upstream, preferred_element_type=jnp.float32)
        return (up_total, down_total), rounded_split_sum(pre_grad, up_weight.T)

    stacked = (earlier_input.reshape(N_FS, group_rows, -1),
               earlier_hidden.reshape(N_FS, group_rows, -1),
               cotangent.reshape(N_FS, group_rows, -1))
    initial = (jnp.zeros(up_weight.shape, jnp.float32), jnp.zeros(down_weight.shape, jnp.float32))
    (up_total, down_total), grads = lax.scan(backward_block, initial, stacked)
    earlier_grad = grads.reshape(row_total, -1)
    return (later_output, later_hidden, earlier_grad,
            up_sum + grad_scale * up_total, down_sum + grad_scale * down_total)
```

```python
import jax
import jax.numpy as jnp
from jax import lax
from jax.sharding import PartitionSpec as P


RING_LIMIT = 16


def contract_last(left_rows, right_rows):
    return lax.dot_general(
        left_rows, right_rows, (((1,), (1,)), ((), ())), preferred_element_type=jnp.float32
    )


def contract_first(left_rows, right_rows):
    return lax.dot_general(
        left_rows, right_rows, (((0,), (0,)), ((), ())), preferred_element_type=jnp.float32
    )


class Ring:
    def __init__(self, axis):
        self.axis = axis
        self.size = lax.axis_size(axis)
        self.order = list(range(0, self.size, 2)) + list(range(1, self.size, 2))[::-1]
        index = lax.axis_index(axis)
        self.place = jnp.where(index % 2 == 0, index // 2, self.size - 1 - index // 2)

    def member(self, shift):
        place = (self.place + shift) % self.size
        evens = (self.size + 1) // 2
        return jnp.where(place < evens, 2 * place, 2 * (self.size - 1 - place) + 1)

    def send(self, piece, step):
        pairs = [
            (self.order[i], self.order[(i + step) % self.size]) for i in range(self.size)
        ]
        return lax.ppermute(piece, self.axis, pairs)


def ring_gather(ring, shard):
    rows = shard.shape[0]
    half = rows // 2
    whole = jnp.zeros((rows * ring.size, shard.shape[1]), shard.dtype)
    whole = lax.dynamic_update_slice(whole, shard, (ring.member(0) * rows, 0))
    upper, lower = shard[:half], shard[half:]
    for step in range(1, ring.size):
        upper, lower = ring.send(upper, 1), ring.send(lower, -1)
        whole = lax.dynamic_update_slice(whole, upper, (ring.member(-step) * rows, 0))
        whole = lax.dynamic_update_slice(whole, lower, (ring.member(step) * rows + half, 0))
    return whole


def ring_scatter(ring, partial):
    rows = partial.shape[0] // ring.size
    half = rows // 2
    width = partial.shape[1]

    def own(shift, offset):
        return lax.dynamic_slice(
            partial, (ring.member(shift) * rows + offset, 0), (half, width)
        )

    upper, lower = own(-1, 0), own(1, half)
    for step in range(1, ring.size):
        upper = ring.send(upper.astype(jnp.bfloat16), 1).astype(jnp.float32)
        lower = ring.send(lower.astype(jnp.bfloat16), -1).astype(jnp.float32)
        upper = upper + own(-1 - step, 0)
        lower = lower + own(1 + step, half)
    return jnp.concatenate([upper, lower], axis=0)


def shards(
    later_input, earlier_input, earlier_hidden, cotangent, up_weight, down_weight, up_sum, down_sum
):
    groups = lax.axis_size("fs")
    grad_scale = float(earlier_input.shape[0] * groups) ** (-0.5)
    if groups <= RING_LIMIT:
        ring = Ring("fs")
        gather = lambda shard: ring_gather(ring, shard)
        scatter = lambda partial: ring_scatter(ring, partial)
    else:
        gather = lambda shard: lax.all_gather(shard, "fs", axis=0, tiled=True)
        scatter = lambda partial: lax.psum_scatter(
            partial, "fs", scatter_dimension=0, tiled=True
        )

    def tp_scatter(partial):
        return lax.psum_scatter(
            partial.astype(jnp.bfloat16), "tp", scatter_dimension=0, tiled=True
        )

    gathered = lax.all_gather(later_input, "tp", axis=0, tiled=True)
    down_full, up_full = gather(down_weight), gather(up_weight)

    lifted = jnp.maximum(earlier_hidden.astype(jnp.float32), 0.0)
    activation = (lifted * lifted).astype(jnp.bfloat16)
    down_partial = contract_first(activation, cotangent)
    pre_grad = (2.0 * contract_last(cotangent, down_full) * lifted).astype(jnp.bfloat16)
    up_partial = contract_first(earlier_input, pre_grad)
    down_total, up_total = scatter(down_partial), scatter(up_partial)

    earlier_grad = tp_scatter(contract_last(pre_grad, up_full))
    later_hidden = jnp.dot(gathered, up_full, preferred_element_type=jnp.float32).astype(
        jnp.bfloat16
    )
    lifted_later = jnp.maximum(later_hidden.astype(jnp.float32), 0.0)
    act_later = (lifted_later * lifted_later).astype(jnp.bfloat16)
    later_output = tp_scatter(jnp.dot(act_later, down_full, preferred_element_type=jnp.float32))
    return (
        later_output,
        later_hidden,
        earlier_grad,
        up_sum + grad_scale * up_total,
        down_sum + grad_scale * down_total,
    )


def solution(mesh):
    in_specs = (
        P(("fs", "tp"), None),
        P("fs", None),
        P("fs", "tp"),
        P("fs", None),
        P("fs", "tp"),
        P(("tp", "fs"), None),
        P("fs", "tp"),
        P(("tp", "fs"), None),
    )
    out_specs = (
        P(("fs", "tp"), None),
        P("fs", "tp"),
        P(("fs", "tp"), None),
        P("fs", "tp"),
        P(("tp", "fs"), None),
    )
    return jax.shard_map(shards, mesh=mesh, in_specs=in_specs, out_specs=out_specs, check_vma=False)
```
